32 devices in a mesh: sp: 16 (over z, y, x), tp: 2 (over core).
Axes of the slice: x: 2, y: 2, z: 4, core: 2. Of those that a mesh axis runs over, the one named last changes fastest.
Arguments:
- tokens: bfloat16 [4096, 2048], P(('sp', 'tp')), may hold values from -6 to 6
- norm_gain: float32 [2048], replicated, may hold values from 0.1 to 1.9
- w_query: bfloat16 [2048, 1024], P('sp', 'tp'), may hold values from -0.125 to 0.125
- w_forget: bfloat16 [2048, 1024], P('sp', 'tp'), may hold values from -0.125 to 0.125
- w_value: bfloat16 [2048, 1024], P('sp', 'tp'), may hold values from -0.125 to 0.125
- w_outgate: bfloat16 [2048, 1024], P('sp', 'tp'), may hold values from -0.125 to 0.125
- leak: float32 [1024], P('tp'), may hold values from 4.8828126e-05 to 0.00024414062
- decay_shift: float32 [4096, 1024], P('sp', 'tp'), may hold values from -1 to 0
- head_gain: float32 [128], replicated, may hold values from 0.1 to 1.9
- w_glu_value: bfloat16 [2048, 2048], P('sp', 'tp'), may hold values from -0.125 to 0.125
- w_glu_gate: bfloat16 [2048, 2048], P('sp', 'tp'), may hold values from -0.125 to 0.125
- conv_kernel: float32 [31, 2048], P(None, 'tp'), may hold values from -20 to 20
- ln_gain: float32 [2048], P('tp'), may hold values from 0.1 to 1.9
- ln_bias: float32 [2048], P('tp'), may hold values from -3 to 3
- w_out_rec: bfloat16 [1024, 2048], P('tp', 'sp'), may hold values from -0.125 to 0.125
- w_out_conv: bfloat16 [2048, 2048], P('tp', 'sp'), may hold values from -0.09375 to 0.09375
Outputs:
- mixed: bfloat16 [4096, 2048], P(('sp', 'tp'))
The draws below stay inside these ranges and needn't reach their ends.
All inputs are finite; a program needn't handle non-finite values.
Results may differ from the reference program's by a relative error of at most 0.019.
Values may be sent and summed in bfloat16 or wider, within the bound.
A program may use at most 64 MiB of HBM per device.

```python
import math
import jax
import jax.numpy as jnp
from jax import lax

D = 2048
HEADS = 8
HEAD_K = 128
HEAD_V = 128
CONV_CH = 2048
KERNEL = 31
BLOCK = 64
TOK_DEV = 256
SEQUENCE_SLOTS = 4096
KEYS_W = 1024
HG_W = 1024
N_TP = 2


def draw_decay_shift(key, part):
    key_width = HEADS * HEAD_K
    generator_seeds = jax.random.split(key, 7)
    fast_share = 0.5
    fast_head = jax.random.uniform(generator_seeds[0], (HEADS,), jnp.float32) < fast_share
    fast_head = jnp.repeat(fast_head, HEAD_K)
    fast_rate = jax.random.uniform(generator_seeds[1], (key_width,), jnp.float32, 0.02, 0.05)
    slow_rate = jax.random.uniform(generator_seeds[2], (key_width,), jnp.float32, 0.2, 0.7) / SEQUENCE_SLOTS
    forgetting_speeds = jnp.where(fast_head, fast_rate, slow_rate)
    block_count = SEQUENCE_SLOTS // TOK_DEV
    magnitude_multiplier = jnp.exp(jax.random.uniform(generator_seeds[3], (block_count,), jnp.float32, -0.7, 0.7))
    magnitude_multiplier = jnp.repeat(magnitude_multiplier, TOK_DEV)
    landscape_jaggedness = jax.random.uniform(generator_seeds[4], (SEQUENCE_SLOTS, key_width), jnp.float32, 0.5, 1.5)
    spike_location = jax.random.randint(generator_seeds[5], (2,), 0, SEQUENCE_SLOTS)
    within_spike_mask = jnp.any(jnp.arange(SEQUENCE_SLOTS)[:, None] == spike_location[None, :], axis=1)
    objective_readings = jax.random.uniform(generator_seeds[6], (key_width,), jnp.float32, 0.22, 0.69)
    payload_matrix_lines = -(forgetting_speeds[None, :] * magnitude_multiplier[:, None] * landscape_jaggedness) - jnp.where(within_spike_mask[:, None], objective_readings[None, :], 0.0)
    return payload_matrix_lines.astype(jnp.float32)


def draw_conv_kernel(key, part):
    generator_seeds = jax.random.split(key, 2)
    channel = jnp.arange(CONV_CH, dtype=jnp.float32) / CONV_CH
    rising = 3.0 ** channel
    spread = 0.5
    jitter = jnp.exp(jax.random.uniform(generator_seeds[0], (CONV_CH,), jnp.float32, -spread, spread))
    payload_matrix_lines = jnp.clip(jax.random.normal(generator_seeds[1], (KERNEL, CONV_CH), jnp.float32), -4.0, 4.0) * KERNEL ** (-0.5)
    return (payload_matrix_lines * rising * jitter).astype(jnp.float32)


def block_scale(stream_key, shape, shards, low, largest):
    loudness = 1.0
    for dim, parts in shards:
        draws = jax.random.uniform(jax.random.fold_in(jax.random.fold_in(stream_key, 6), dim), (parts,), jnp.float32, low / len(shards), largest / len(shards))
        loudness = loudness * jnp.repeat(jnp.exp(draws), shape[dim] // parts).reshape((-1,) + (1,) * (len(shape) - 1 - dim))
    return loudness


def scatter_about(stream_key, shape, scale, most, cuts=(), kind=jnp.bfloat16):
    array = scale * jax.random.normal(stream_key, shape, jnp.float32)
    if cuts:
        array = array * block_scale(stream_key, shape, cuts, -0.22, 0.18)
    return jnp.clip(array, -most, most).astype(kind)


def setup_inputs(seed: int = 0) -> dict:
    splits = jax.random.split(jax.random.key(seed), 17)
    return {
        "tokens": scatter_about(splits[0], (SEQUENCE_SLOTS, D), 1.0, 6.0, ((0, 32),)),
        "norm_gain": jnp.clip(1.0 + 0.18 * jax.random.normal(splits[1], (D,), jnp.float32), 0.1, 1.9),
        "w_query": scatter_about(splits[2], (D, KEYS_W), D ** -0.5, 0.125, ((0, 16), (1, 2))),
        "w_forget": scatter_about(splits[3], (D, KEYS_W), D ** -0.5, 0.125, ((0, 16), (1, 2))),
        "w_value": scatter_about(splits[4], (D, HG_W), D ** -0.5, 0.125, ((0, 16), (1, 2))),
        "w_outgate": scatter_about(splits[5], (D, HG_W), D ** -0.5, 0.125, ((0, 16), (1, 2))),
        "leak": jnp.clip(jnp.exp(math.log(0.00024414062) - 1.609438 * jax.random.uniform(splits[6], (KEYS_W,), jnp.float32) ** block_scale(splits[6], (KEYS_W,), ((0, 2),), -0.2, 0.2)), 4.882812572759576e-05, 0.00024414062),
        "decay_shift": draw_decay_shift(jax.random.fold_in(splits[16], 71), 0),
        "head_gain": jnp.clip(1.0 + 0.18 * jax.random.normal(splits[8], (HEAD_V,), jnp.float32), 0.1, 1.9),
        "w_glu_value": scatter_about(splits[9], (D, CONV_CH), D ** -0.5, 0.125, ((0, 16), (1, 2))),
        "w_glu_gate": scatter_about(splits[10], (D, CONV_CH), D ** -0.5, 0.125, ((0, 16), (1, 2))),
        "conv_kernel": draw_conv_kernel(jax.random.fold_in(splits[16], 71), 0),
        "ln_gain": jnp.clip(1.0 + 0.18 * jax.random.normal(splits[12], (CONV_CH,), jnp.float32), 0.1, 1.9),
        "ln_bias": scatter_about(splits[13], (CONV_CH,), 0.5, 3.0, ((0, 2),), jnp.float32),
        "w_out_rec": scatter_about(splits[14], (HG_W, D), (2 * HG_W) ** -0.5, 0.125, ((0, 2), (1, 16))),
        "w_out_conv": scatter_about(splits[15], (CONV_CH, D), (2 * CONV_CH) ** -0.5, 0.09375, ((0, 2), (1, 16))),
    }


exact_precision = lax.Precision.HIGHEST

def project(normed, weight):
    return jnp.dot(normed, weight, preferred_element_type=jnp.float32).astype(jnp.bfloat16)

def recurrence(queries, in_gate, payload_matrix_lines, log_decay):
    block_count = SEQUENCE_SLOTS // BLOCK

    def split_blocks(tensor):
        return tensor.reshape(block_count, BLOCK, HEADS, tensor.shape[-1])
    causal = jnp.tril(jnp.ones((BLOCK, BLOCK), jnp.float32))

    def advance(state_list, inputs):
        query_block, key_block, value_block, a_block = inputs
        cumulative_sum = jnp.cumsum(a_block, axis=0)
        gap_logs = jnp.minimum(cumulative_sum[:, None] - cumulative_sum[None, :], 0.0)
        decays = jnp.exp(gap_logs) * causal[:, :, None, None]
        scores = jnp.einsum('thk,shk,tshk->hts', query_block, key_block, decays, precision=exact_precision)
        within = jnp.einsum('hts,shv->thv', scores, value_block, precision=exact_precision)
        carried_state = jnp.einsum('aub,ubd->aud', query_block * jnp.exp(cumulative_sum), state_list, precision=exact_precision)
        block_finish = cumulative_sum[-1]
        added_terms = jnp.einsum('fjb,fji->jbi', key_block * jnp.exp(block_finish[None] - cumulative_sum), value_block, precision=exact_precision)
        state_list = jnp.exp(block_finish)[:, :, None] * state_list + added_terms
        return (state_list, within + carried_state)
    initial = jnp.zeros((HEADS, HEAD_K, HEAD_V), jnp.float32)
    _, outputs = lax.scan(advance, initial, (split_blocks(queries), split_blocks(in_gate), split_blocks(payload_matrix_lines), split_blocks(log_decay)))
    return outputs.reshape(SEQUENCE_SLOTS, HEADS, HEAD_V)

def reference(tokens, norm_gain, w_query, w_forget, w_value, w_outgate, leak, decay_shift, head_gain, w_glu_value, w_glu_gate, conv_kernel, ln_gain, ln_bias, w_out_rec, w_out_conv):
    values_in = tokens.astype(jnp.float32)
    row_scale = lax.rsqrt(lax.optimization_barrier(jnp.mean(values_in * values_in, axis=1, keepdims=True)) + 1e-06)
    normed = (values_in * row_scale * norm_gain).astype(jnp.bfloat16)
    query_pre = project(normed, w_query)
    forget_pre = project(normed, w_forget)
    value_pre = project(normed, w_value)
    gate_pre = project(normed, w_outgate)
    glu_value_pre = project(normed, w_glu_value)
    glu_gate_pre = project(normed, w_glu_gate)
    queries = jax.nn.silu(query_pre.astype(jnp.float32))
    in_gate = leak * jax.nn.sigmoid(-forget_pre.astype(jnp.float32))
    log_decay = jnp.log1p(-in_gate) + decay_shift
    recurrence_step = recurrence(queries.reshape(SEQUENCE_SLOTS, HEADS, HEAD_K), in_gate.reshape(SEQUENCE_SLOTS, HEADS, HEAD_K), value_pre.astype(jnp.float32).reshape(SEQUENCE_SLOTS, HEADS, HEAD_V), log_decay.reshape(SEQUENCE_SLOTS, HEADS, HEAD_K))
    scaling = lax.rsqrt(lax.optimization_barrier(jnp.mean(recurrence_step * recurrence_step, axis=2, keepdims=True)) + 1e-06)
    gate_act = jax.nn.silu(gate_pre.astype(jnp.float32)).reshape(SEQUENCE_SLOTS, HEADS, HEAD_V)
    head_out = (recurrence_step * scaling * head_gain * gate_act).reshape(SEQUENCE_SLOTS, HG_W).astype(jnp.bfloat16)
    glu = (glu_value_pre.astype(jnp.float32) * jax.nn.sigmoid(glu_gate_pre.astype(jnp.float32))).astype(jnp.bfloat16)
    padded = jnp.pad(glu.astype(jnp.float32), ((KERNEL - 1, 0), (0, 0)))
    conv_sum = jnp.zeros((SEQUENCE_SLOTS, CONV_CH), jnp.float32)
    for tap_index in range(KERNEL):
        conv_sum = conv_sum + conv_kernel[tap_index] * padded[tap_index:tap_index + SEQUENCE_SLOTS]
    row_mean = lax.optimization_barrier(jnp.mean(conv_sum, axis=1, keepdims=True))
    centered = conv_sum - row_mean
    row_var = lax.optimization_barrier(jnp.mean(centered * centered, axis=1, keepdims=True))
    conv_out = jax.nn.silu(centered * lax.rsqrt(row_var + 1e-05) * ln_gain + ln_bias).astype(jnp.bfloat16)
    rec_group = HG_W // N_TP
    conv_group = CONV_CH // N_TP
    summed = jnp.zeros((SEQUENCE_SLOTS, D), jnp.float32)
    for group_index in range(N_TP):
        rec_cols = slice(group_index * rec_group, (group_index + 1) * rec_group)
        conv_cols = slice(group_index * conv_group, (group_index + 1) * conv_group)
        partial_value = jnp.dot(head_out[:, rec_cols], w_out_rec[rec_cols], preferred_element_type=jnp.float32)
        partial_value = partial_value + jnp.dot(conv_out[:, conv_cols], w_out_conv[conv_cols], preferred_element_type=jnp.float32)
        rounded = lax.optimization_barrier(partial_value.astype(jnp.bfloat16))
        summed = summed + rounded.astype(jnp.float32)
    return summed.astype(jnp.bfloat16)
```

```python
import jax
import jax.numpy as jnp
from jax import lax
from jax.experimental import pallas as pl
from jax.experimental.pallas import tpu as pltpu
from jax.sharding import PartitionSpec as P

HEAD_K = 128
HEAD_V = 128
KERNEL = 31
HALO = 32
BLOCK = 64
MESH = pl.DeviceIdType.MESH


exact_precision = lax.Precision.HIGHEST


def exchange(x, kind, group, scatter, collective_id):
    lines = lax.axis_size("sp") // group
    cores = lax.axis_size("tp")
    count = {"line": lines, "plane": group, "core": cores, "all": group * cores}[kind]
    shape = x.shape if scatter else (count,) + x.shape
    if count == 1:
        return x.reshape(shape)

    def body(x_ref, o_ref, send_sem, recv_sem, local_sem):
        sp, core = lax.axis_index("sp"), lax.axis_index("tp")
        line, spot = sp // group, sp % group

        def where(m):
            return {
                "line": lambda: (m * group + spot, core),
                "plane": lambda: (line * group + m, core),
                "core": lambda: (sp, m),
                "all": lambda: (line * group + m // cores, m % cores),
            }[kind]()

        me = {"line": line, "plane": spot, "core": core, "all": spot * cores + core}[kind]
        others = [lax.rem(me + d, count) for d in range(1, count)]
        barrier = pltpu.get_barrier_semaphore()
        for other in others:
            pl.semaphore_signal(barrier, inc=1, device_id=where(other), device_id_type=MESH)
        pl.semaphore_wait(barrier, count - 1)
        copies = []
        for d, other in enumerate(others):
            copy = pltpu.make_async_remote_copy(
                src_ref=x_ref.at[other] if scatter else x_ref,
                dst_ref=o_ref.at[me],
                send_sem=send_sem.at[d],
                recv_sem=recv_sem.at[d],
                device_id=where(other),
                device_id_type=MESH,
            )
            copy.start()
            copies.append(copy)
        own = pltpu.make_async_copy(x_ref.at[me] if scatter else x_ref, o_ref.at[me], local_sem)
        own.start()
        own.wait()
        for copy in copies:
            copy.wait()

    return pl.pallas_call(
        body,
        out_shape=jax.ShapeDtypeStruct(shape, x.dtype),
        in_specs=[pl.BlockSpec(memory_space=pltpu.VMEM)],
        out_specs=pl.BlockSpec(memory_space=pltpu.VMEM),
        scratch_shapes=[
            pltpu.SemaphoreType.DMA((count,)),
            pltpu.SemaphoreType.DMA((count,)),
            pltpu.SemaphoreType.DMA,
        ],
        compiler_params=pltpu.CompilerParams(collective_id=collective_id, has_side_effects=True),
    )(x)


def spread(pieces, rows, group, collective_id):
    slots = lax.axis_size("sp")
    lines = slots // group
    cores = lax.axis_size("tp")
    peers = group * cores

    def body(
        w_ref, t_ref, w_all, t_all,
        plane_send, up_send, down_send, w_recv, t_send, t_recv, local_sem,
    ):
        sp, core = lax.axis_index("sp"), lax.axis_index("tp")
        line, spot = sp // group, sp % group
        seat = spot * cores + core
        has_up, has_down = line + 1 < lines, line > 0
        barrier = pltpu.get_barrier_semaphore()

        def greet(device):
            pl.semaphore_signal(barrier, inc=1, device_id=device, device_id_type=MESH)

        def place(m):
            return (line * group + m // cores, m % cores)

        others = [lax.rem(seat + d, peers) for d in range(1, peers)]
        for other in others:
            greet(place(other))

        @pl.when(has_up)
        def _():
            greet((sp + group, core))

        @pl.when(has_down)
        def _():
            greet((sp - group, core))

        met = peers - 1 + has_up.astype(jnp.int32) + has_down.astype(jnp.int32)
        pl.semaphore_wait(barrier, met)

        def remote(src, dst, send_sem, recv_sem, device):
            return pltpu.make_async_remote_copy(
                src_ref=src, dst_ref=dst, send_sem=send_sem, recv_sem=recv_sem,
                device_id=device, device_id_type=MESH,
            )

        own = pltpu.make_async_copy(w_ref.at[spot], w_all.at[sp], local_sem.at[0])
        own.start()
        started = []
        for d in range(1, group):
            to = lax.rem(spot + d, group)
            copy = remote(
                w_ref.at[to], w_all.at[sp], plane_send.at[d], w_recv.at[sp],
                (line * group + to, core),
            )
            copy.start()
            started.append(copy)
        own_rows = pltpu.make_async_copy(t_ref, t_all.at[seat], local_sem.at[1])
        own_rows.start()
        row_copies = []
        for d, other in enumerate(others):
            copy = remote(t_ref, t_all.at[seat], t_send.at[d], t_recv.at[d], place(other))
            copy.start()
            row_copies.append(copy)

        def up(slot):
            return remote(
                w_all.at[slot], w_all.at[slot], up_send.at[slot], w_recv.at[slot],
                (sp + group, core),
            )

        def down(slot):
            return remote(
                w_all.at[slot], w_all.at[slot], down_send.at[slot], w_recv.at[slot],
                (sp - group, core),
            )

        def arrive(slot, device):
            remote(
                w_all.at[slot], w_all.at[slot], up_send.at[slot], w_recv.at[slot], device
            ).wait_recv()

        own.wait()
        for d in range(lines):
            for k in range(group):
                if d == 0:
                    slot = line * group + lax.rem(spot + k, group)
                    if k > 0:
                        arrive(slot, (slot, core))

                    @pl.when(has_up)
                    def _():
                        up(slot).start()

                    @pl.when(has_down)
                    def _():
                        down(slot).start()
                else:
                    low = (line - d) * group + lax.rem(spot + k, group)
                    high = (line + d) * group + lax.rem(spot + k, group)

                    @pl.when(line >= d)
                    def _():
                        arrive(low, (sp - group, core))

                        @pl.when(has_up)
                        def _():
                            up(low).start()

                    @pl.when(line + d < lines)
                    def _():
                        arrive(high, (sp + group, core))

                        @pl.when(has_down)
                        def _():
                            down(high).start()

        own_rows.wait()
        for copy in row_copies:
            copy.wait()
        for copy in started:
            copy.wait_send()
        for d in range(lines):
            for k in range(group):
                low = (line - d) * group + k
                high = (line + d) * group + k

                @pl.when((line >= d) & has_up)
                def _():
                    up(low).wait_send()

                @pl.when((line + d < lines) & has_down)
                def _():
                    down(high).wait_send()

    return pl.pallas_call(
        body,
        out_shape=(
            jax.ShapeDtypeStruct((slots,) + pieces.shape[1:], pieces.dtype),
            jax.ShapeDtypeStruct((peers,) + rows.shape, rows.dtype),
        ),
        in_specs=[pl.BlockSpec(memory_space=pltpu.VMEM)] * 2,
        out_specs=[pl.BlockSpec(memory_space=pltpu.VMEM)] * 2,
        scratch_shapes=[
            pltpu.SemaphoreType.DMA((group,)),
            pltpu.SemaphoreType.DMA((slots,)),
            pltpu.SemaphoreType.DMA((slots,)),
            pltpu.SemaphoreType.DMA((slots,)),
            pltpu.SemaphoreType.DMA((peers,)),
            pltpu.SemaphoreType.DMA((peers,)),
            pltpu.SemaphoreType.DMA((2,)),
        ],
        compiler_params=pltpu.CompilerParams(
            collective_id=collective_id, has_side_effects=True, vmem_limit_bytes=48 * 2**20
        ),
    )(pieces, rows)


def depthwise(extended, taps):
    rows = extended.shape[0] - HALO
    channels = extended.shape[1]
    step = 64
    wide = 128

    def body(x_ref, k_ref, o_ref):
        for column in range(0, channels, wide):
            here = slice(column, column + wide)

            @pl.loop(0, rows // step)
            def _(turn):
                base = pl.multiple_of(turn * step, step)
                chunk = x_ref[pl.ds(base, step + HALO), here]
                total = jnp.zeros((step, wide), jnp.float32)
                for phase in range(8):
                    turned = chunk if phase == 0 else pltpu.roll(chunk, step + HALO - phase, 0)
                    for start in range(0, HALO + 8, 8):
                        j = start + phase - (HALO - (KERNEL - 1))
                        if 0 <= j < KERNEL:
                            total = total + k_ref[j : j + 1, here] * turned[start : start + step]
                o_ref[pl.ds(base, step), here] = total

    return pl.pallas_call(
        body,
        out_shape=jax.ShapeDtypeStruct((rows, channels), jnp.float32),
        in_specs=[pl.BlockSpec(memory_space=pltpu.VMEM)] * 2,
        out_specs=pl.BlockSpec(memory_space=pltpu.VMEM),
        cost_estimate=pl.CostEstimate(
            flops=2 * KERNEL * rows * channels, bytes_accessed=8 * rows * channels, transcendentals=0
        ),
    )(extended, taps)


def normalize(row_block, norm_gain):
    values_in = row_block.astype(jnp.float32)
    row_scale = lax.rsqrt(jnp.mean(values_in * values_in, axis=1, keepdims=True) + 1e-06)
    return (values_in * row_scale * norm_gain).astype(jnp.bfloat16)


def recurrence(queries, in_gate, value, log_decay, group):
    rows, width = queries.shape
    blocks = rows // BLOCK
    q, k, v, a = (
        t.reshape(blocks, BLOCK, t.shape[1]) for t in (queries, in_gate, value, log_decay)
    )
    causal = jnp.tril(jnp.ones((BLOCK, BLOCK), jnp.float32))
    running = jnp.einsum("ts,nsk->ntk", causal, a, precision=exact_precision)
    finish = running[:, -1]
    q_in = (q * jnp.exp(running)).astype(jnp.bfloat16)
    k_out = (k * jnp.exp(-running)).astype(jnp.bfloat16)
    k_end = (k * jnp.exp(finish[:, None] - running)).astype(jnp.bfloat16)
    scores = jnp.einsum("ntk,nsk->nts", q_in, k_out, preferred_element_type=jnp.float32)
    within = jnp.einsum(
        "nts,nsv->ntv", (scores * causal).astype(jnp.bfloat16), v, preferred_element_type=jnp.float32
    )
    added = jnp.einsum("nsk,nsv->nkv", k_end, v, preferred_element_type=jnp.float32)
    after = jnp.cumsum(finish[::-1], axis=0)[::-1]
    total = after[0]
    tail = jnp.exp(after - finish)
    local_state = jnp.sum(tail[..., None] * added, axis=0)
    sent = jnp.concatenate([local_state, jnp.broadcast_to(total[None], (8, width))], axis=0)
    gathered = exchange(sent, "line", group, False, 1)
    line = lax.axis_index("sp") // group
    state = jnp.zeros_like(local_state)
    for m in range(gathered.shape[0]):
        grown = jnp.exp(gathered[m, width])[:, None] * state + gathered[m, :width]
        state = jnp.where(m < line, grown, state)
    before = []
    factor = jnp.exp(finish)
    for n in range(blocks):
        before.append(state.astype(jnp.bfloat16))
        state = factor[n][:, None] * state + added[n]
    carried = jnp.einsum(
        "ntk,nkv->ntv", q_in, jnp.stack(before), preferred_element_type=jnp.float32
    )
    return (within + carried).reshape(rows, value.shape[1])


def on_device(
    tokens,
    norm_gain,
    w_query,
    w_forget,
    w_value,
    w_outgate,
    leak,
    decay_shift,
    head_gain,
    w_glu_value,
    w_glu_gate,
    conv_kernel,
    ln_gain,
    ln_bias,
    w_out_rec,
    w_out_conv,
):
    bf16 = jnp.bfloat16
    slots, cores = lax.axis_size("sp"), lax.axis_size("tp")
    group = w_query.shape[1] // HEAD_K
    spot = lax.axis_index("sp") % group
    depth = w_query.shape[0]
    width = w_out_rec.shape[1]
    channels = w_glu_value.shape[1] // group
    inner = HEAD_V + channels
    total_width = 4 * HEAD_K + 2 * channels

    def by_spot(weight):
        return weight.reshape(depth, group, -1)

    pieces = jnp.concatenate(
        [by_spot(w) for w in (w_query, w_forget, w_value, w_outgate, w_glu_value, w_glu_gate)],
        axis=2,
    ).transpose(1, 0, 2)
    out_pieces = jnp.concatenate(
        [w_out_rec.reshape(group, HEAD_V, width), w_out_conv.reshape(group, channels, width)], axis=1
    )
    folds = total_width // width
    out_pieces = (
        out_pieces.reshape(group, folds, inner // folds, width)
        .transpose(0, 2, 1, 3)
        .reshape(group, inner // folds, total_width)
    )
    everything, normed = spread(
        jnp.concatenate([pieces, out_pieces], axis=1), normalize(tokens, norm_gain), group, 0
    )
    shift_all = exchange(
        decay_shift.reshape(decay_shift.shape[0], group, HEAD_K).transpose(1, 0, 2),
        "plane", group, True, 2,
    )
    rows = normed.shape[0] * normed.shape[1]
    normed = normed.reshape(rows, normed.shape[2])
    shift = shift_all.reshape(rows, HEAD_K)
    full_in = everything[:, :depth].reshape(slots * depth, total_width)
    full_out = (
        everything[:, depth:]
        .reshape(slots, inner // folds, folds, width)
        .transpose(2, 1, 0, 3)
        .reshape(inner, slots * width)
    )
    joined = jnp.dot(normed, full_in, preferred_element_type=jnp.float32).astype(bf16)
    query_pre, forget_pre, value_pre, gate_pre = (
        joined[:, n * HEAD_K : (n + 1) * HEAD_K] for n in range(4)
    )
    glu_value_pre = joined[:, 4 * HEAD_K : 4 * HEAD_K + channels]
    glu_gate_pre = joined[:, 4 * HEAD_K + channels :]

    glu = (
        glu_value_pre.astype(jnp.float32) * jax.nn.sigmoid(glu_gate_pre.astype(jnp.float32))
    ).astype(bf16)
    rim = lax.ppermute(
        glu[rows - HALO :], "sp", [(s, s + group) for s in range(slots - group)]
    )
    extended = jnp.concatenate([rim, glu], axis=0).astype(jnp.float32)
    mine = lambda t: lax.dynamic_slice_in_dim(t, spot * channels, channels, t.ndim - 1)
    conv_sum = depthwise(extended, mine(conv_kernel))
    sums = jnp.stack([jnp.sum(conv_sum, axis=1), jnp.sum(conv_sum * conv_sum, axis=1)])
    sums = jnp.sum(exchange(sums, "all", group, False, 3), axis=0)
    channel_count = channels * group * cores
    row_mean = sums[0][:, None] / channel_count
    row_var = sums[1][:, None] / channel_count - row_mean * row_mean
    conv_out = jax.nn.silu(
        (conv_sum - row_mean) * lax.rsqrt(row_var + 1e-05) * mine(ln_gain) + mine(ln_bias)
    ).astype(bf16)

    queries = jax.nn.silu(query_pre.astype(jnp.float32))
    own_leak = lax.dynamic_slice_in_dim(leak, spot * HEAD_K, HEAD_K, 0)
    in_gate = own_leak * jax.nn.sigmoid(-forget_pre.astype(jnp.float32))
    log_decay = jnp.log1p(-in_gate) + shift
    recur = recurrence(queries, in_gate, value_pre, log_decay, group)
    scaling = lax.rsqrt(jnp.mean(recur * recur, axis=1, keepdims=True) + 1e-06)
    head_out = (recur * scaling * head_gain * jax.nn.silu(gate_pre.astype(jnp.float32))).astype(bf16)

    partial = jnp.dot(
        jnp.concatenate([head_out, conv_out], axis=1), full_out, preferred_element_type=jnp.float32
    ).astype(bf16)
    own_rows = tokens.shape[0]
    by_core = partial.reshape(group, cores, own_rows, -1).transpose(1, 0, 2, 3)
    by_plane = exchange(by_core, "core", group, True, 4)
    by_plane = jnp.sum(by_plane.astype(jnp.float32), axis=0).astype(bf16)
    back = exchange(by_plane, "plane", group, True, 5)
    return jnp.sum(back.astype(jnp.float32), axis=0).astype(bf16)


def solution(mesh):
    placed = (
        P(("sp", "tp"), None),
        P(),
        P("sp", "tp"),
        P("sp", "tp"),
        P("sp", "tp"),
        P("sp", "tp"),
        P("tp"),
        P("sp", "tp"),
        P(),
        P("sp", "tp"),
        P("sp", "tp"),
        P(None, "tp"),
        P("tp"),
        P("tp"),
        P("tp", "sp"),
        P("tp", "sp"),
    )
    return jax.shard_map(
        on_device, mesh=mesh, in_specs=placed, out_specs=P(("sp", "tp"), None), check_vma=False
    )
```

```python
import jax
import jax.numpy as jnp
from jax import lax
from jax.experimental import pallas as pl
from jax.experimental.pallas import tpu as pltpu
from jax.sharding import PartitionSpec as P

HEAD_K = 128
HEAD_V = 128
KERNEL = 31
HALO = 32
BLOCK = 64
MESH = pl.DeviceIdType.MESH


exact_precision = lax.Precision.HIGHEST


def exchange(x, kind, group, scatter, collective_id):
    lines = lax.axis_size("sp") // group
    cores = lax.axis_size("tp")
    count = {"line": lines, "plane": group, "core": cores, "all": group * cores}[kind]
    shape = x.shape if scatter else (count,) + x.shape
    if count == 1:
        return x.reshape(shape)

    def body(x_ref, o_ref, send_sem, recv_sem, local_sem):
        sp, core = lax.axis_index("sp"), lax.axis_index("tp")
        line, spot = sp // group, sp % group

        def where(m):
            return {
                "line": lambda: (m * group + spot, core),
                "plane": lambda: (line * group + m, core),
                "core": lambda: (sp, m),
                "all": lambda: (line * group + m // cores, m % cores),
            }[kind]()

        me = {"line": line, "plane": spot, "core": core, "all": spot * cores + core}[kind]
        others = [lax.rem(me + d, count) for d in range(1, count)]
        barrier = pltpu.get_barrier_semaphore()
        for other in others:
            pl.semaphore_signal(barrier, inc=1, device_id=where(other), device_id_type=MESH)
        pl.semaphore_wait(barrier, count - 1)
        copies = []
        for d, other in enumerate(others):
            copy = pltpu.make_async_remote_copy(
                src_ref=x_ref.at[other] if scatter else x_ref,
                dst_ref=o_ref.at[me],
                send_sem=send_sem.at[d],
                recv_sem=recv_sem.at[d],
                device_id=where(other),
                device_id_type=MESH,
            )
            copy.start()
            copies.append(copy)
        own = pltpu.make_async_copy(x_ref.at[me] if scatter else x_ref, o_ref.at[me], local_sem)
        own.start()
        own.wait()
        for copy in copies:
            copy.wait()

    return pl.pallas_call(
        body,
        out_shape=jax.ShapeDtypeStruct(shape, x.dtype),
        in_specs=[pl.BlockSpec(memory_space=pltpu.VMEM)],
        out_specs=pl.BlockSpec(memory_space=pltpu.VMEM),
        scratch_shapes=[
            pltpu.SemaphoreType.DMA((count,)),
            pltpu.SemaphoreType.DMA((count,)),
            pltpu.SemaphoreType.DMA,
        ],
        compiler_params=pltpu.CompilerParams(collective_id=collective_id, has_side_effects=True),
    )(x)


def spread(pieces, rows, group, collective_id):
    slots = lax.axis_size("sp")
    lines = slots // group
    cores = lax.axis_size("tp")
    peers = group * cores

    def body(
        w_ref, t_ref, w_all, t_all,
        plane_send, up_send, down_send, w_recv, t_send, t_recv, local_sem,
    ):
        sp, core = lax.axis_index("sp"), lax.axis_index("tp")
        line, spot = sp // group, sp % group
        seat = spot * cores + core
        has_up, has_down = line + 1 < lines, line > 0
        barrier = pltpu.get_barrier_semaphore()

        def greet(device):
            pl.semaphore_signal(barrier, inc=1, device_id=device, device_id_type=MESH)

        def place(m):
            return (line * group + m // cores, m % cores)

        others = [lax.rem(seat + d, peers) for d in range(1, peers)]
        for other in others:
            greet(place(other))

        @pl.when(has_up)
        def _():
            greet((sp + group, core))

        @pl.when(has_down)
        def _():
            greet((sp - group, core))

        met = peers - 1 + has_up.astype(jnp.int32) + has_down.astype(jnp.int32)
        pl.semaphore_wait(barrier, met)

        def remote(src, dst, send_sem, recv_sem, device):
            return pltpu.make_async_remote_copy(
                src_ref=src, dst_ref=dst, send_sem=send_sem, recv_sem=recv_sem,
                device_id=device, device_id_type=MESH,
            )

        own = pltpu.make_async_copy(w_ref.at[spot], w_all.at[sp], local_sem.at[0])
        own.start()
        started = []
        for d in range(1, group):
            to = lax.rem(spot + d, group)
            copy = remote(
                w_ref.at[to], w_all.at[sp], plane_send.at[d], w_recv.at[sp],
                (line * group + to, core),
            )
            copy.start()
            started.append(copy)
        own_rows = pltpu.make_async_copy(t_ref, t_all.at[seat], local_sem.at[1])
        own_rows.start()
        row_copies = []
        for d, other in enumerate(others):
            copy = remote(t_ref, t_all.at[seat], t_send.at[d], t_recv.at[d], place(other))
            copy.start()
            row_copies.append(copy)

        def up(slot):
            return remote(
                w_all.at[slot], w_all.at[slot], up_send.at[slot], w_recv.at[slot],
                (sp + group, core),
            )

        def down(slot):
            return remote(
                w_all.at[slot], w_all.at[slot], down_send.at[slot], w_recv.at[slot],
                (sp - group, core),
            )

        def arrive(slot, device):
            remote(
                w_all.at[slot], w_all.at[slot], up_send.at[slot], w_recv.at[slot], device
            ).wait_recv()

        own.wait()
        for d in range(lines):
            for k in range(group):
                if d == 0:
                    slot = line * group + lax.rem(spot + k, group)
                    if k > 0:
                        arrive(slot, (slot, core))

                    @pl.when(has_up)
                    def _():
                        up(slot).start()

                    @pl.when(has_down)
                    def _():
                        down(slot).start()
                else:
                    low = (line - d) * group + lax.rem(spot + k, group)
                    high = (line + d) * group + lax.rem(spot + k, group)

                    @pl.when(line >= d)
                    def _():
                        arrive(low, (sp - group, core))

                        @pl.when(has_up)
                        def _():
                            up(low).start()

                    @pl.when(line + d < lines)
                    def _():
                        arrive(high, (sp + group, core))

                        @pl.when(has_down)
                        def _():
                            down(high).start()

        own_rows.wait()
        for copy in row_copies:
            copy.wait()
        for copy in started:
            copy.wait_send()
        for d in range(lines):
            for k in range(group):
                low = (line - d) * group + k
                high = (line + d) * group + k

                @pl.when((line >= d) & has_up)
                def _():
                    up(low).wait_send()

                @pl.when((line + d < lines) & has_down)
                def _():
                    down(high).wait_send()

    return pl.pallas_call(
        body,
        out_shape=(
            jax.ShapeDtypeStruct((slots,) + pieces.shape[1:], pieces.dtype),
            jax.ShapeDtypeStruct((peers,) + rows.shape, rows.dtype),
        ),
        in_specs=[pl.BlockSpec(memory_space=pltpu.VMEM)] * 2,
        out_specs=[pl.BlockSpec(memory_space=pltpu.VMEM)] * 2,
        scratch_shapes=[
            pltpu.SemaphoreType.DMA((group,)),
            pltpu.SemaphoreType.DMA((slots,)),
            pltpu.SemaphoreType.DMA((slots,)),
            pltpu.SemaphoreType.DMA((slots,)),
            pltpu.SemaphoreType.DMA((peers,)),
            pltpu.SemaphoreType.DMA((peers,)),
            pltpu.SemaphoreType.DMA((2,)),
        ],
        compiler_params=pltpu.CompilerParams(
            collective_id=collective_id, has_side_effects=True, vmem_limit_bytes=48 * 2**20
        ),
    )(pieces, rows)


def depthwise(extended, taps):
    rows = extended.shape[0] - HALO
    channels = extended.shape[1]
    step = 64
    wide = 128

    def body(x_ref, k_ref, o_ref):
        for column in range(0, channels, wide):
            here = slice(column, column + wide)

            @pl.loop(0, rows // step)
            def _(turn):
                base = pl.multiple_of(turn * step, step)
                chunk = x_ref[pl.ds(base, step + HALO), here]
                total = jnp.zeros((step, wide), jnp.float32)
                for phase in range(8):
                    turned = chunk if phase == 0 else pltpu.roll(chunk, step + HALO - phase, 0)
                    for start in range(0, HALO + 8, 8):
                        j = start + phase - (HALO - (KERNEL - 1))
                        if 0 <= j < KERNEL:
                            total = total + k_ref[j : j + 1, here] * turned[start : start + step]
                o_ref[pl.ds(base, step), here] = total

    return pl.pallas_call(
        body,
        out_shape=jax.ShapeDtypeStruct((rows, channels), jnp.float32),
        in_specs=[pl.BlockSpec(memory_space=pltpu.VMEM)] * 2,
        out_specs=pl.BlockSpec(memory_space=pltpu.VMEM),
        cost_estimate=pl.CostEstimate(
            flops=2 * KERNEL * rows * channels, bytes_accessed=8 * rows * channels, transcendentals=0
        ),
    )(extended, taps)


def normalize(row_block, norm_gain):
    values_in = row_block.astype(jnp.float32)
    row_scale = lax.rsqrt(jnp.mean(values_in * values_in, axis=1, keepdims=True) + 1e-06)
    return (values_in * row_scale * norm_gain).astype(jnp.bfloat16)


def carry_through(q_in, added, factor, state):
    blocks = q_in.shape[0]

    def body(q_ref, add_ref, factor_ref, state_ref, o_ref):
        now = state_ref[...]
        for n in range(blocks):
            o_ref[n] = jnp.dot(
                q_ref[n], now.astype(jnp.bfloat16), preferred_element_type=jnp.float32
            )
            now = factor_ref[:, n : n + 1] * now + add_ref[n]

    return pl.pallas_call(
        body,
        out_shape=jax.ShapeDtypeStruct(q_in.shape[:2] + state.shape[1:], jnp.float32),
        in_specs=[pl.BlockSpec(memory_space=pltpu.VMEM)] * 4,
        out_specs=pl.BlockSpec(memory_space=pltpu.VMEM),
    )(q_in, added, factor, state)


def recurrence(queries, in_gate, value, log_decay, group):
    rows, width = queries.shape
    blocks = rows // BLOCK
    q, k, v, a = (
        t.reshape(blocks, BLOCK, t.shape[1]) for t in (queries, in_gate, value, log_decay)
    )
    causal = jnp.tril(jnp.ones((BLOCK, BLOCK), jnp.float32))
    running = jnp.einsum("ts,nsk->ntk", causal, a, precision=exact_precision)
    finish = running[:, -1]
    q_in = (q * jnp.exp(running)).astype(jnp.bfloat16)
    k_out = (k * jnp.exp(-running)).astype(jnp.bfloat16)
    k_end = (k * jnp.exp(finish[:, None] - running)).astype(jnp.bfloat16)
    scores = jnp.einsum("ntk,nsk->nts", q_in, k_out, preferred_element_type=jnp.float32)
    within = jnp.einsum(
        "nts,nsv->ntv", (scores * causal).astype(jnp.bfloat16), v, preferred_element_type=jnp.float32
    )
    added = jnp.einsum("nsk,nsv->nkv", k_end, v, preferred_element_type=jnp.float32)
    after = jnp.cumsum(finish[::-1], axis=0)[::-1]
    total = after[0]
    tail = jnp.exp(after - finish)
    local_state = jnp.sum(tail[..., None] * added, axis=0)
    sent = jnp.concatenate([local_state, jnp.broadcast_to(total[None], (8, width))], axis=0)
    gathered = exchange(sent, "line", group, False, 1)
    line = lax.axis_index("sp") // group
    state = jnp.zeros_like(local_state)
    for m in range(gathered.shape[0]):
        grown = jnp.exp(gathered[m, width])[:, None] * state + gathered[m, :width]
        state = jnp.where(m < line, grown, state)
    carried = carry_through(q_in, added, jnp.exp(finish).T, state)
    return (within + carried).reshape(rows, value.shape[1])


def on_device(
    tokens,
    norm_gain,
    w_query,
    w_forget,
    w_value,
    w_outgate,
    leak,
    decay_shift,
    head_gain,
    w_glu_value,
    w_glu_gate,
    conv_kernel,
    ln_gain,
    ln_bias,
    w_out_rec,
    w_out_conv,
):
    bf16 = jnp.bfloat16
    slots, cores = lax.axis_size("sp"), lax.axis_size("tp")
    group = w_query.shape[1] // HEAD_K
    spot = lax.axis_index("sp") % group
    depth = w_query.shape[0]
    width = w_out_rec.shape[1]
    channels = w_glu_value.shape[1] // group
    inner = HEAD_V + channels
    total_width = 4 * HEAD_K + 2 * channels

    def by_spot(weight):
        return weight.reshape(depth, group, -1)

    pieces = jnp.concatenate(
        [by_spot(w) for w in (w_query, w_forget, w_value, w_outgate, w_glu_value, w_glu_gate)],
        axis=2,
    ).transpose(1, 0, 2)
    out_pieces = jnp.concatenate(
        [w_out_rec.reshape(group, HEAD_V, width), w_out_conv.reshape(group, channels, width)], axis=1
    )
    folds = total_width // width
    out_pieces = (
        out_pieces.reshape(group, folds, inner // folds, width)
        .transpose(0, 2, 1, 3)
        .reshape(group, inner // folds, total_width)
    )
    everything, normed = spread(
        jnp.concatenate([pieces, out_pieces], axis=1), normalize(tokens, norm_gain), group, 0
    )
    shift_all = exchange(
        decay_shift.reshape(decay_shift.shape[0], group, HEAD_K).transpose(1, 0, 2),
        "plane", group, True, 2,
    )
    rows = normed.shape[0] * normed.shape[1]
    normed = normed.reshape(rows, normed.shape[2])
    shift = shift_all.reshape(rows, HEAD_K)
    full_in = everything[:, :depth].reshape(slots * depth, total_width)
    full_out = (
        everything[:, depth:]
        .reshape(slots, inner // folds, folds, width)
        .transpose(2, 1, 0, 3)
        .reshape(inner, slots * width)
    )
    joined = jnp.dot(normed, full_in, preferred_element_type=jnp.float32).astype(bf16)
    query_pre, forget_pre, value_pre, gate_pre = (
        joined[:, n * HEAD_K : (n + 1) * HEAD_K] for n in range(4)
    )
    glu_value_pre = joined[:, 4 * HEAD_K : 4 * HEAD_K + channels]
    glu_gate_pre = joined[:, 4 * HEAD_K + channels :]

    glu = (
        glu_value_pre.astype(jnp.float32) * jax.nn.sigmoid(glu_gate_pre.astype(jnp.float32))
    ).astype(bf16)
    rim = lax.ppermute(
        glu[rows - HALO :], "sp", [(s, s + group) for s in range(slots - group)]
    )
    extended = jnp.concatenate([rim, glu], axis=0).astype(jnp.float32)
    mine = lambda t: lax.dynamic_slice_in_dim(t, spot * channels, channels, t.ndim - 1)
    conv_sum = depthwise(extended, mine(conv_kernel))
    sums = jnp.stack([jnp.sum(conv_sum, axis=1), jnp.sum(conv_sum * conv_sum, axis=1)])
    sums = jnp.sum(exchange(sums, "all", group, False, 3), axis=0)
    channel_count = channels * group * cores
    row_mean = sums[0][:, None] / channel_count
    row_var = sums[1][:, None] / channel_count - row_mean * row_mean
    conv_out = jax.nn.silu(
        (conv_sum - row_mean) * lax.rsqrt(row_var + 1e-05) * mine(ln_gain) + mine(ln_bias)
    ).astype(bf16)

    queries = jax.nn.silu(query_pre.astype(jnp.float32))
    own_leak = lax.dynamic_slice_in_dim(leak, spot * HEAD_K, HEAD_K, 0)
    in_gate = own_leak * jax.nn.sigmoid(-forget_pre.astype(jnp.float32))
    log_decay = jnp.log1p(-in_gate) + shift
    recur = recurrence(queries, in_gate, value_pre, log_decay, group)
    scaling = lax.rsqrt(jnp.mean(recur * recur, axis=1, keepdims=True) + 1e-06)
    head_out = (recur * scaling * head_gain * jax.nn.silu(gate_pre.astype(jnp.float32))).astype(bf16)

    partial = jnp.dot(
        jnp.concatenate([head_out, conv_out], axis=1), full_out, preferred_element_type=jnp.float32
    ).astype(bf16)
    own_rows = tokens.shape[0]
    by_core = partial.reshape(group, cores, own_rows, -1).transpose(1, 0, 2, 3)
    by_plane = exchange(by_core, "core", group, True, 4)
    by_plane = jnp.sum(by_plane.astype(jnp.float32), axis=0).astype(bf16)
    back = exchange(by_plane, "plane", group, True, 5)
    return jnp.sum(back.astype(jnp.float32), axis=0).astype(bf16)


def solution(mesh):
    placed = (
        P(("sp", "tp"), None),
        P(),
        P("sp", "tp"),
        P("sp", "tp"),
        P("sp", "tp"),
        P("sp", "tp"),
        P("tp"),
        P("sp", "tp"),
        P(),
        P("sp", "tp"),
        P("sp", "tp"),
        P(None, "tp"),
        P("tp"),
        P("tp"),
        P("tp", "sp"),
        P("tp", "sp"),
    )
    return jax.shard_map(
        on_device, mesh=mesh, in_specs=placed, out_specs=P(("sp", "tp"), None), check_vma=False
    )
```
